32 devices in a mesh: grp: 1, ep: 16 (over z, y, x), tp: 2 (over core).
Axes of the slice: x: 2, y: 2, z: 4, core: 2. Of those that a mesh axis runs over, the one named last changes fastest.
Arguments:
- tokens: bfloat16 [2048, 2048], P(('grp', 'ep', 'tp')), may hold values from -6 to 6
- norm_gain: float32 [2048], replicated, may hold values from 0.1 to 1.9
- expert_ids: int32 [2048, 2], P(('grp', 'ep', 'tp')), may hold values from 0 to 3, all different within a row; in each aligned block of 64 rows (0 to 63, 64 to 127, ...) at most 42 rows name the same one
- gate_weights: float32 [2048, 2], P(('grp', 'ep', 'tp')), may hold values from 0.2 to 1
- w_gate: bfloat16 [2048, 28672], P(None, ('ep', 'tp')), may hold values from -0.125 to 0.125
- w_up: bfloat16 [2048, 28672], P(None, ('ep', 'tp')), may hold values from -0.125 to 0.125
- w_down: bfloat16 [28672, 2048], P(('ep', 'tp')), may hold values from -0.0625 to 0.0625
Outputs:
- mixed: bfloat16 [2048, 2048], P(('grp', 'ep', 'tp'))
The draws below stay inside these ranges and needn't reach their ends.
Inputs may be any that keep to these rules, and one draw needn't show every extreme that they name: `expert_ids`: each token names 2 different experts. Among the rows of one device no expert is named by more than 42 rows, a bound that some blocks reach; every expert is named somewhere.
All inputs are finite; a program needn't handle non-finite values.
Results may differ from the reference program's by a relative error of at most 0.0095.
Values may be sent and summed in bfloat16 or wider, within the bound.
A program may use at most 192 MiB of HBM per device.

```python
import math
import jax
import jax.numpy as jnp
import numpy as np
from jax import lax

D = 2048
FF = 7168
TOPK = 2
GROUP = 4
TOK_DEV = 64
EXPERTS = 4
CAP = 42
TOKENS = 2048
N_EP = 16
N_TP = 2


def steps_of(own_key, shape, pieces, low, largest):
    level = 1.0
    for dim, shards_of in pieces:
        heights = jax.random.uniform(jax.random.fold_in(jax.random.fold_in(own_key, 6), dim), (shards_of,), jnp.float32, low / len(pieces), largest / len(pieces))
        level = level * jnp.repeat(jnp.exp(heights), shape[dim] // shards_of).reshape((-1,) + (1,) * (len(shape) - 1 - dim))
    return level


def routed_block(stream_key, own, number, rows, amount, top, limit, lean):
    ranking = jax.random.permutation(stream_key, amount)
    crowded, common = load_shares(amount, rows * top, limit, lean, True), load_shares(amount, rows * top, limit, lean, False)
    places = jnp.arange(amount)

    def named(lengths, turn):
        used = int((lengths > 0).sum())
        fixed = max(1, used // 4)
        passed = fixed + (places - fixed + turn * (used - fixed)) % max(1, amount - fixed)
        return jnp.zeros((amount,), jnp.int32).at[ranking[jnp.where(places < fixed, places, passed)]].set(jnp.asarray(lengths, jnp.int32))

    lengths = jnp.where(number % 4 == 0, named(crowded, number // 4), named(common, number - number // 4 - 1))
    mixed = jax.random.permutation(jax.random.fold_in(own, 3), amount)
    source_of, sink = mixed[0:amount // 2 * 2:2], mixed[1:amount // 2 * 2:2]
    room = jnp.minimum(lengths[source_of] - 1, limit - lengths[sink]) // 2
    room = jnp.where((source_of == ranking[0]) | (sink == ranking[0]) | (lengths[sink] == 0), 0, jnp.maximum(room, 0))
    passed = jax.random.randint(jax.random.fold_in(own, 4), (amount // 2,), 0, 1 << 20) % (room + 1)
    lengths = lengths.at[source_of].add(-passed).at[sink].add(passed)
    members = jnp.searchsorted(jnp.cumsum(lengths), jnp.arange(rows * top), side="right").astype(jnp.int32)
    table = members.reshape(top, rows).T
    table = table[jax.random.permutation(jax.random.fold_in(own, 1), rows)]
    turn = jax.random.randint(jax.random.fold_in(own, 2), (rows, 1), 0, top)
    return jnp.take_along_axis(table, (jnp.arange(top)[None, :] + turn) % top, axis=1)


def load_shares(count, total, bound, slope, full):
    portions = [(1 << 20) // math.isqrt(standing ** slope) + 1 for standing in range(1, count + 1)]
    largest = bound if full else min(bound, max(-(-total // count), total * portions[0] // sum(portions)))
    least = 1 if total - largest >= count - 1 else 0
    counts, spare = [largest] + [least] * (count - 1), total - largest - least * (count - 1)
    while spare > 0:
        free = [i for i in range(1, count) if counts[i] < largest] or [i for i in range(1, count) if counts[i] < bound]
        whole, left = sum([portions[i] for i in free]), spare
        for i in free:
            addition = min(bound - counts[i], max(1, left * portions[i] // whole), spare)
            counts[i] = counts[i] + addition
            spare = spare - addition
    return np.array(counts)


def gaussian(rng, dims, scale, bound, shards=(), kind=jnp.bfloat16):
    gain = steps_of(rng, dims, shards, -0.22, 0.18) if shards else 1.0
    result = jax.random.normal(rng, dims, jnp.float32) * scale * gain
    return jnp.minimum(jnp.maximum(result, -bound), bound).astype(kind)


def setup_inputs(seed: int = 0, part: int = 0) -> dict:
    key_of = jax.random.split(jax.random.key(seed), 8)
    part_splits = jax.random.split(jax.random.fold_in(key_of[7], part), 8)
    tokens = gaussian(part_splits[0], (TOKENS, D), 1.0, 6.0, ((0, 32),))
    norm_gain = jnp.clip(1.0 + 0.18 * jax.random.normal(key_of[1], (D,), jnp.float32), 0.1, 1.9)
    expert_ids_keys = jax.random.split(jax.random.fold_in(part_splits[2], 1), TOKENS // TOK_DEV)
    expert_ids_turns = jax.random.permutation(jax.random.fold_in(part_splits[2], 3), TOKENS // TOK_DEV)
    expert_ids = jax.vmap(lambda own, number: routed_block(jax.random.fold_in(part_splits[2], 2), own, number, TOK_DEV, EXPERTS, TOPK, CAP, 2))(expert_ids_keys, expert_ids_turns).reshape((TOKENS, TOPK))
    gate_weights = jnp.clip(0.2 + 0.8 * jax.random.uniform(part_splits[3], (TOKENS, TOPK), jnp.float32) ** steps_of(part_splits[3], (TOKENS, TOPK), ((0, 32),), -0.2, 0.2), 0.2, 1.0)
    w_gate = gaussian(key_of[4], (D, EXPERTS * FF), D ** -0.5, 0.125, ((1, 32),))
    w_up = gaussian(key_of[5], (D, EXPERTS * FF), D ** -0.5, 0.125, ((1, 32),))
    w_down = gaussian(key_of[6], (EXPERTS * FF, D), FF ** -0.5, 0.0625, ((0, 32),))
    return {"tokens": tokens, "norm_gain": norm_gain, "expert_ids": expert_ids, "gate_weights": gate_weights, "w_gate": w_gate, "w_up": w_up, "w_down": w_down}


def layer_norm(tokens, norm_gain):
    values = tokens.astype(jnp.float32)
    center = lax.optimization_barrier(jnp.mean(values, -1, keepdims=True))
    spread = lax.optimization_barrier(jnp.mean(jnp.square(values - center), -1, keepdims=True))
    return ((values - center) * lax.rsqrt(spread + 1e-05) * norm_gain).astype(jnp.bfloat16)

def rounded(values):
    return lax.optimization_barrier(values.astype(jnp.bfloat16)).astype(jnp.float32)

def reference(tokens, norm_gain, expert_ids, gate_weights, w_gate, w_up, w_down):
    normed = layer_norm(tokens, norm_gain)
    padded = jnp.concatenate([normed, jnp.zeros((1, D), jnp.bfloat16)], 0)
    flat_ids = expert_ids.reshape(-1).astype(jnp.int32)
    matches = (flat_ids[:, None] == jnp.arange(EXPERTS, dtype=jnp.int32)[None, :]).astype(jnp.int32)
    position = lax.optimization_barrier(jnp.sum((jnp.cumsum(matches, 0) - 1) * matches, 1)).astype(jnp.int32)
    buffer_rows = N_EP * N_TP * CAP
    source = (jnp.arange(TOKENS * TOPK, dtype=jnp.int32) // TOPK).astype(jnp.int32)
    slot_table = jnp.full((EXPERTS, buffer_rows), TOKENS, jnp.int32).at[flat_ids, position].set(source)
    block_width = FF // (GROUP * N_TP)

    def one_expert(expert_index):
        picked_rows = padded[slot_table[expert_index]]
        first_col = (expert_index * FF).astype(jnp.int32)
        gate_cols = lax.dynamic_slice_in_dim(w_gate, first_col, FF, 1)
        up_cols = lax.dynamic_slice_in_dim(w_up, first_col, FF, 1)
        down_rows = lax.dynamic_slice_in_dim(w_down, first_col, FF, 0)
        running = jnp.zeros((buffer_rows, D), jnp.float32)
        for member in range(GROUP):
            paired = jnp.zeros((buffer_rows, D), jnp.float32)
            for side_index in range(N_TP):
                offset = (member * N_TP + side_index) * block_width
                gate_part = jnp.dot(picked_rows, gate_cols[:, offset:offset + block_width], preferred_element_type=jnp.float32)
                up_part = jnp.dot(picked_rows, up_cols[:, offset:offset + block_width], preferred_element_type=jnp.float32)
                hidden_part = (jax.nn.silu(gate_part) * up_part).astype(jnp.bfloat16)
                paired = paired + rounded(jnp.dot(hidden_part, down_rows[offset:offset + block_width], preferred_element_type=jnp.float32))
            running = running + rounded(paired)
        return running
    results = lax.map(one_expert, jnp.arange(EXPERTS, dtype=jnp.int32))
    picked = results[flat_ids, position] * gate_weights.reshape(-1)[:, None]
    return lax.optimization_barrier(jnp.sum(picked.reshape(TOKENS, TOPK, D), 1)).astype(jnp.bfloat16)
```

```python
import functools

import jax
import jax.numpy as jnp
from jax import lax
from jax.experimental import pallas as pl
from jax.experimental.pallas import tpu as pltpu
from jax.sharding import PartitionSpec as P

GROUP = 4
MESH = pl.DeviceIdType.MESH
F32, BF16 = jnp.float32, jnp.bfloat16
Z_IN, A_X, A_Y, R_X, R_Y, P_X0, P_X1, P_Y0, P_Y1, Q_X, Q_Y, Z_OUT = range(12)
COPIES = 12


def kernel(
    experts, cap, cols,
    tokens_ref, gain_ref, ids_ref, gates_ref, wg_ref, wu_ref, wd_ref, out_ref,
    wg, wu, wd, packed, xbuf, hidden, ybuf, rxa, rxb, cbuf, fbuf, zrx,
    send, recv, wsend, wrecv, wlocal,
):
    rows, width = tokens_ref.shape
    block = wg_ref.shape[1]
    half = width // 2
    grp, ep, core = lax.axis_index("grp"), lax.axis_index("ep"), lax.axis_index("tp")
    e, m = ep // GROUP, ep % GROUP
    left, right = pl.ds(0, half), pl.ds(half, half)

    def at(expert, member):
        return (grp, lax.rem(expert + 2 * experts, experts) * GROUP + member, core)

    mx = m + 1 - 2 * (m % 2)
    my = m + 2 - 4 * (m // 2)
    xdev, ydev = at(e, mx), at(e, my)
    other = (grp, ep, 1 - core)
    slots = experts * cap

    local = [
        pltpu.make_async_copy(wg_ref, wg.at[:, pl.ds(0, block)], wlocal.at[0]),
        pltpu.make_async_copy(wu_ref, wu.at[:, pl.ds(0, block)], wlocal.at[1]),
        pltpu.make_async_copy(wd_ref, wd.at[pl.ds(0, block)], wlocal.at[2]),
    ]
    for copy in local:
        copy.start()

    barrier = pltpu.get_barrier_semaphore()
    partners = [xdev, ydev, other] + [at(e - k, m) for k in range(1, experts)]
    for device in partners:
        pl.semaphore_signal(barrier, inc=1, device_id=device, device_id_type=MESH)

    values = tokens_ref[...].astype(F32)
    center = jnp.mean(values, -1, keepdims=True)
    spread = jnp.mean(jnp.square(values - center), -1, keepdims=True)
    normed = ((values - center) * lax.rsqrt(spread + 1e-05) * gain_ref[...]).astype(BF16)

    lane = lax.broadcasted_iota(jnp.int32, (rows, slots), 1)
    place = lane
    number = jnp.zeros((rows, slots), jnp.int32) + e
    for k in range(1, experts):
        past = (lane >= k * cap).astype(jnp.int32)
        place = place - cap * past
        number = number - past
    number = jnp.where(number < 0, number + experts, number)
    picks = ids_ref.shape[1]
    match = [(ids_ref[:, i : i + 1] == number).astype(F32) for i in range(picks)]
    named = functools.reduce(lambda a, b: a + b, match)
    before = (
        lax.broadcasted_iota(jnp.int32, (rows, rows), 1)
        < lax.broadcasted_iota(jnp.int32, (rows, rows), 0)
    ).astype(F32)
    position = jnp.dot(before.astype(BF16), named.astype(BF16), preferred_element_type=F32)
    taken = jnp.abs(position - place.astype(F32)) < 0.5
    chosen = [jnp.where(taken, one, 0.0).astype(BF16) for one in match]
    onehot = jnp.where(taken, named, 0.0)
    packed[...] = lax.dot_general(
        onehot.T.astype(BF16), normed, (((1,), (0,)), ((), ())), preferred_element_type=F32
    ).astype(BF16)
    xbuf[0, pl.ds(0, cap)] = packed[pl.ds(0, cap)]

    pl.semaphore_wait(barrier, len(partners))

    def remote(k, kind, src, dst, device):
        return pltpu.make_async_remote_copy(
            src_ref=src, dst_ref=dst, send_sem=send.at[k * COPIES + kind],
            recv_sem=recv.at[k * COPIES + kind], device_id=device, device_id_type=MESH,
        )

    def xs(k, j):
        return xbuf.at[k, pl.ds(j * cap, cap)]

    def ys(k, j, c):
        return ybuf.at[k, pl.ds(j * cap, cap), c]

    copies = {}
    for k in range(experts):
        if k:
            copies[k, Z_IN] = remote(k, Z_IN, packed.at[pl.ds(k * cap, cap)], xs(k, 0), at(e - k, m))
            copies[k, Z_OUT] = remote(k, Z_OUT, fbuf.at[k], zrx.at[pl.ds(k * cap, cap)], at(e + k, m))
        copies[k, A_X] = remote(k, A_X, xs(k, 0), xs(k, 1), xdev)
        copies[k, A_Y] = remote(k, A_Y, xs(k, 0), xs(k, 2), ydev)
        copies[k, R_Y] = remote(
            k, R_Y, xbuf.at[k, pl.ds(cap, cap), left], xbuf.at[k, pl.ds(3 * cap, cap), left], ydev)
        copies[k, R_X] = remote(
            k, R_X, xbuf.at[k, pl.ds(2 * cap, cap), right], xbuf.at[k, pl.ds(3 * cap, cap), right], xdev)
        copies[k, P_X0] = remote(k, P_X0, ys(k, 1, left), rxa.at[k, 0, :, left], xdev)
        copies[k, P_X1] = remote(k, P_X1, ys(k, 3, left), rxa.at[k, 1, :, left], xdev)
        copies[k, P_Y0] = remote(k, P_Y0, ys(k, 2, right), rxa.at[k, 0, :, right], ydev)
        copies[k, P_Y1] = remote(k, P_Y1, ys(k, 3, right), rxa.at[k, 1, :, right], ydev)
        copies[k, Q_Y] = remote(k, Q_Y, cbuf.at[k, :, left], rxb.at[k, :, left], ydev)
        copies[k, Q_X] = remote(k, Q_X, cbuf.at[k, :, right], rxb.at[k, :, right], xdev)

    def spread_out(k):
        if k:
            copies[k, Z_IN].wait_recv()
        copies[k, A_X].start()
        copies[k, A_Y].start()

    def relay(k):
        copies[k, A_X].wait_recv()
        copies[k, R_Y].start()
        copies[k, A_Y].wait_recv()
        copies[k, R_X].start()

    def compute(k):
        copies[k, R_Y].wait_recv()
        copies[k, R_X].wait_recv()

        def up(n, carry):
            at_n = pl.ds(pl.multiple_of(n * cols, cols), cols)
            x = xbuf[k]
            g = jnp.dot(x, wg[:, at_n], preferred_element_type=F32)
            u = jnp.dot(x, wu[:, at_n], preferred_element_type=F32)
            hidden[:, at_n] = (jax.nn.silu(g) * u).astype(BF16)
            return carry

        lax.fori_loop(0, 2 * block // cols, up, 0)

        def down(n, carry):
            at_n = pl.ds(pl.multiple_of(n * cols, cols), cols)
            ybuf[k, :, at_n] = jnp.dot(
                hidden[...], wd[:, at_n], preferred_element_type=F32
            ).astype(BF16)
            return carry

        lax.fori_loop(0, width // cols, down, 0)
        for kind in (P_X1, P_Y1, P_X0, P_Y0):
            copies[k, kind].start()

    def middle(k):
        copies[k, P_X1].wait_recv()
        cbuf[k, :, left] = (
            ybuf[k, pl.ds(2 * cap, cap), left].astype(F32) + rxa[k, 1, :, left].astype(F32)
        ).astype(BF16)
        copies[k, Q_Y].start()
        copies[k, P_Y1].wait_recv()
        cbuf[k, :, right] = (
            ybuf[k, pl.ds(cap, cap), right].astype(F32) + rxa[k, 1, :, right].astype(F32)
        ).astype(BF16)
        copies[k, Q_X].start()

    def finish(k):
        for kind in (P_X0, P_Y0, Q_X, Q_Y):
            copies[k, kind].wait_recv()
        total = (
            ybuf[k, pl.ds(0, cap)].astype(F32) + rxa[k, 0].astype(F32) + rxb[k].astype(F32)
        ).astype(BF16)
        if k:
            fbuf[k] = total
            copies[k, Z_OUT].start()
        else:
            zrx[pl.ds(0, cap)] = total

    for k in range(1, experts):
        copies[k, Z_IN].start()
    spread_out(0)
    weights = []
    for i, (src, dst) in enumerate(
        ((wg_ref, wg.at[:, pl.ds(block, block)]), (wu_ref, wu.at[:, pl.ds(block, block)]),
         (wd_ref, wd.at[pl.ds(block, block)]))
    ):
        weights.append(pltpu.make_async_remote_copy(
            src_ref=src, dst_ref=dst, send_sem=wsend.at[i], recv_sem=wrecv.at[i],
            device_id=other, device_id_type=MESH))
        weights[-1].start()
    for k in range(1, experts):
        spread_out(k)
        if k < experts - 1:
            relay(k - 1)
    for copy in local:
        copy.wait()
    for copy in weights:
        copy.wait_recv()
    for k in range(experts):
        compute(k)
        if k + experts - 2 < experts:
            relay(k + experts - 2)
        if k >= 1:
            middle(k - 1)
        if k >= 2:
            finish(k - 2)
    middle(experts - 1)
    finish(experts - 2)
    finish(experts - 1)

    for k in range(1, experts):
        copies[k, Z_OUT].wait_recv()

    def combine(n, carry):
        at_n = pl.ds(pl.multiple_of(n * cols, cols), cols)
        z = zrx[:, at_n]
        total = jnp.zeros((rows, cols), F32)
        for i in range(picks):
            total = total + gates_ref[:, i : i + 1] * jnp.dot(
                chosen[i], z, preferred_element_type=F32)
        out_ref[:, at_n] = total.astype(BF16)
        return carry

    lax.fori_loop(0, width // cols, combine, 0)
    for copy in copies.values():
        copy.wait_send()
    for copy in weights:
        copy.wait_send()


def per_device(tokens, norm_gain, expert_ids, gate_weights, w_gate, w_up, w_down):
    ep_devices = lax.axis_size("ep")
    rows, width = tokens.shape
    block = w_gate.shape[1]
    picks = expert_ids.shape[1]
    experts = ep_devices // GROUP
    capacity = max(2, min(rows, rows * picks * 4 // (3 * experts)))
    cap = -(-capacity // 16) * 16
    vmem = pl.BlockSpec(memory_space=pltpu.VMEM)
    hbm = pl.BlockSpec(memory_space=pl.ANY)
    chunk = GROUP * cap
    return pl.pallas_call(
        functools.partial(kernel, experts, cap, 256),
        out_shape=jax.ShapeDtypeStruct((rows, width), BF16),
        in_specs=[vmem] * 4 + [hbm] * 3,
        out_specs=vmem,
        scratch_shapes=[
            pltpu.VMEM((width, 2 * block), BF16),
            pltpu.VMEM((width, 2 * block), BF16),
            pltpu.VMEM((2 * block, width), BF16),
            pltpu.VMEM((experts * cap, width), BF16),
            pltpu.VMEM((experts, chunk, width), BF16),
            pltpu.VMEM((chunk, 2 * block), BF16),
            pltpu.VMEM((experts, chunk, width), BF16),
            pltpu.VMEM((experts, 2, cap, width), BF16),
            pltpu.VMEM((experts, cap, width), BF16),
            pltpu.VMEM((experts, cap, width), BF16),
            pltpu.VMEM((experts, cap, width), BF16),
            pltpu.VMEM((experts * cap, width), BF16),
            pltpu.SemaphoreType.DMA((experts * COPIES,)),
            pltpu.SemaphoreType.DMA((experts * COPIES,)),
            pltpu.SemaphoreType.DMA((3,)),
            pltpu.SemaphoreType.DMA((3,)),
            pltpu.SemaphoreType.DMA((3,)),
        ],
        compiler_params=pltpu.CompilerParams(
            collective_id=0, has_side_effects=True, vmem_limit_bytes=60 * 1024 * 1024),
    )(tokens, norm_gain.reshape(1, width), expert_ids, gate_weights, w_gate, w_up, w_down)


def solution(mesh):
    rows = P(("grp", "ep", "tp"), None)
    return jax.shard_map(
        per_device, mesh=mesh,
        in_specs=(rows, P(), rows, rows, P(None, ("ep", "tp")), P(None, ("ep", "tp")),
                  P(("ep", "tp"), None)),
        out_specs=rows, check_vma=False,
    )
```

```python
import functools

import jax
import jax.numpy as jnp
from jax import lax
from jax.experimental import pallas as pl
from jax.experimental.pallas import tpu as pltpu
from jax.sharding import PartitionSpec as P

GROUP = 4
MESH = pl.DeviceIdType.MESH
F32, BF16 = jnp.float32, jnp.bfloat16
Z_IN, A_X, A_Y, R_X, R_Y, P_X0, P_X1, P_Y0, P_Y1, Q_X, Q_Y, Z_OUT = range(12)
COPIES = 12


def kernel(
    experts, cap, cols,
    tokens_ref, gain_ref, ids_ref, gates_ref, wg_ref, wu_ref, wd_ref, out_ref,
    wg, wu, wd, packed, xbuf, hidden, ybuf, rxa, rxb, cbuf, fbuf, zrx,
    send, recv, wsend, wrecv, wlocal,
):
    rows, width = tokens_ref.shape
    block = wg_ref.shape[1]
    half = width // 2
    grp, ep, core = lax.axis_index("grp"), lax.axis_index("ep"), lax.axis_index("tp")
    e, m = ep // GROUP, ep % GROUP
    left, right = pl.ds(0, half), pl.ds(half, half)

    def at(expert, member):
        return (grp, expert * GROUP + member, core)

    edge = jnp.minimum(e, experts - 1 - e)
    toward = 1 - 2 * (e // (experts // 2))
    order = [e]
    for i in range(1, experts):
        paired = i <= 2 * edge
        step = (i + 1) // 2 if i % 2 else -(i // 2)
        order.append(jnp.where(paired, e + step, e + toward * (i - edge)))

    mx = m + 1 - 2 * (m % 2)
    my = m + 2 - 4 * (m // 2)
    xdev, ydev = at(e, mx), at(e, my)
    other = (grp, ep, 1 - core)
    slots = experts * cap

    local = [
        pltpu.make_async_copy(wg_ref, wg.at[:, pl.ds(0, block)], wlocal.at[0]),
        pltpu.make_async_copy(wu_ref, wu.at[:, pl.ds(0, block)], wlocal.at[1]),
        pltpu.make_async_copy(wd_ref, wd.at[pl.ds(0, block)], wlocal.at[2]),
    ]
    for copy in local:
        copy.start()

    barrier = pltpu.get_barrier_semaphore()
    partners = [xdev, ydev, other] + [at(plane, m) for plane in order[1:]]
    for device in partners:
        pl.semaphore_signal(barrier, inc=1, device_id=device, device_id_type=MESH)

    values = tokens_ref[...].astype(F32)
    center = jnp.mean(values, -1, keepdims=True)
    spread = jnp.mean(jnp.square(values - center), -1, keepdims=True)
    normed = ((values - center) * lax.rsqrt(spread + 1e-05) * gain_ref[...]).astype(BF16)

    row = lax.broadcasted_iota(jnp.int32, (slots, rows), 0)
    number = jnp.zeros((slots, rows), jnp.int32)
    for k in range(1, experts):
        number = number + (row >= k * cap).astype(jnp.int32)
    place = row - cap * number
    picks = ids_ref.shape[0]
    match = [(ids_ref[i : i + 1, :] == number).astype(F32) for i in range(picks)]
    named = functools.reduce(lambda a, b: a + b, match)
    before = (
        lax.broadcasted_iota(jnp.int32, (rows, rows), 0)
        < lax.broadcasted_iota(jnp.int32, (rows, rows), 1)
    ).astype(F32)
    position = jnp.dot(named.astype(BF16), before.astype(BF16), preferred_element_type=F32)
    taken = jnp.abs(position - place.astype(F32)) < 0.5
    chosen = [jnp.where(taken, one, 0.0) for one in match]
    gates = [
        jnp.sum((one * gates_ref[i : i + 1, :]).T, 1, keepdims=True)
        for i, one in enumerate(chosen)
    ]
    chosen = [one.T.astype(BF16) for one in chosen]
    onehot = jnp.where(taken, named, 0.0).astype(BF16)
    packed[...] = jnp.dot(onehot, normed, preferred_element_type=F32).astype(BF16)
    own = pl.ds(pl.multiple_of(e * cap, cap), cap)
    xbuf[e, pl.ds(0, cap)] = packed[own]

    pl.semaphore_wait(barrier, len(partners))

    turn = iter(range(2 * experts * COPIES))

    def remote(k, kind, src, dst, device):
        return pltpu.make_async_remote_copy(
            src_ref=src, dst_ref=dst, send_sem=send.at[next(turn)],
            recv_sem=recv.at[k * COPIES + kind], device_id=device, device_id_type=MESH,
        )

    def xs(k, j):
        return xbuf.at[k, pl.ds(j * cap, cap)]

    def ys(k, j, c):
        return ybuf.at[k, pl.ds(j * cap, cap), c]

    copies, arrivals = {}, {}
    for k in range(experts):
        k_ = order[k]
        if k:
            block_k = pl.ds(pl.multiple_of(k_ * cap, cap), cap)
            arrivals[k, Z_IN] = remote(k_, Z_IN, packed.at[block_k], xs(k_, 0), at(k_, m))
            copies[k, Z_IN] = remote(e, Z_IN, packed.at[block_k], xs(e, 0), at(k_, m))
            arrivals[k, Z_OUT] = remote(k_, Z_OUT, fbuf.at[k_], zrx.at[block_k], at(k_, m))
            copies[k, Z_OUT] = remote(e, Z_OUT, fbuf.at[k_], zrx.at[own], at(k_, m))
        copies[k, A_X] = remote(k_, A_X, xs(k_, 0), xs(k_, 1), xdev)
        copies[k, A_Y] = remote(k_, A_Y, xs(k_, 0), xs(k_, 2), ydev)
        copies[k, R_Y] = remote(k_, R_Y, xbuf.at[k_, pl.ds(cap, cap), left], xbuf.at[k_, pl.ds(3 * cap, cap), left], ydev)
        copies[k, R_X] = remote(k_, R_X, xbuf.at[k_, pl.ds(2 * cap, cap), right], xbuf.at[k_, pl.ds(3 * cap, cap), right], xdev)
        copies[k, P_X0] = remote(k_, P_X0, ys(k_, 1, left), rxa.at[k_, 0, :, left], xdev)
        copies[k, P_X1] = remote(k_, P_X1, ys(k_, 3, left), rxa.at[k_, 1, :, left], xdev)
        copies[k, P_Y0] = remote(k_, P_Y0, ys(k_, 2, right), rxa.at[k_, 0, :, right], ydev)
        copies[k, P_Y1] = remote(k_, P_Y1, ys(k_, 3, right), rxa.at[k_, 1, :, right], ydev)
        copies[k, Q_Y] = remote(k_, Q_Y, cbuf.at[k_, :, left], rxb.at[k_, :, left], ydev)
        copies[k, Q_X] = remote(k_, Q_X, cbuf.at[k_, :, right], rxb.at[k_, :, right], xdev)

    def spread_out(k):
        if k:
            arrivals[k, Z_IN].wait_recv()
        copies[k, A_X].start()
        copies[k, A_Y].start()

    def relay(k):
        copies[k, A_X].wait_recv()
        copies[k, R_Y].start()
        copies[k, A_Y].wait_recv()
        copies[k, R_X].start()

    def compute(k):
        k_ = order[k]
        copies[k, R_Y].wait_recv()
        copies[k, R_X].wait_recv()

        def up(n, carry):
            at_n = pl.ds(pl.multiple_of(n * cols, cols), cols)
            x = xbuf[k_]
            g = jnp.dot(x, wg[:, at_n], preferred_element_type=F32)
            u = jnp.dot(x, wu[:, at_n], preferred_element_type=F32)
            hidden[:, at_n] = (jax.nn.silu(g) * u).astype(BF16)
            return carry

        if k == turns[0]:
            for i in range(2):
                local[i].wait()
                weights[i].wait_recv()
        lax.fori_loop(0, 2 * block // cols, up, 0, unroll=True)
        if k == turns[0]:
            local[2].wait()
            weights[2].wait_recv()

        def down(n, carry):
            at_n = pl.ds(pl.multiple_of(n * cols, cols), cols)
            ybuf[k_, :, at_n] = jnp.dot(
                hidden[...], wd[:, at_n], preferred_element_type=F32
            ).astype(BF16)
            return carry

        lax.fori_loop(0, width // cols, down, 0, unroll=True)
        for kind in (P_X1, P_Y1, P_X0, P_Y0):
            copies[k, kind].start()

    def middle(k):
        k_ = order[k]
        copies[k, P_X1].wait_recv()
        cbuf[k_, :, left] = (
            ybuf[k_, pl.ds(2 * cap, cap), left].astype(F32) + rxa[k_, 1, :, left].astype(F32)
        ).astype(BF16)
        copies[k, Q_Y].start()
        copies[k, P_Y1].wait_recv()
        cbuf[k_, :, right] = (
            ybuf[k_, pl.ds(cap, cap), right].astype(F32) + rxa[k_, 1, :, right].astype(F32)
        ).astype(BF16)
        copies[k, Q_X].start()

    def finish(k):
        k_ = order[k]
        for kind in (P_X0, P_Y0, Q_X, Q_Y):
            copies[k, kind].wait_recv()
        total = (
            ybuf[k_, pl.ds(0, cap)].astype(F32) + rxa[k_, 0].astype(F32) + rxb[k_].astype(F32)
        ).astype(BF16)
        if k:
            fbuf[k_] = total
            copies[k, Z_OUT].start()
        else:
            zrx[own] = total

    for k in range(1, experts):
        copies[k, Z_IN].start()
    spread_out(0)
    weights = []
    for i, (src, dst) in enumerate(
        ((wg_ref, wg.at[:, pl.ds(block, block)]), (wu_ref, wu.at[:, pl.ds(block, block)]),
         (wd_ref, wd.at[pl.ds(block, block)]))
    ):
        weights.append(pltpu.make_async_remote_copy(
            src_ref=src, dst_ref=dst, send_sem=wsend.at[i], recv_sem=wrecv.at[i],
            device_id=other, device_id_type=MESH))
        weights[-1].start()
    turns = [*range(1, experts), 0]
    relay(0)
    for k in range(1, experts):
        spread_out(k)
        if k > 1:
            relay(k - 1)
    for i, k in enumerate(turns):
        compute(k)
        if i == 0:
            relay(experts - 1)
        if i >= 1:
            middle(turns[i - 1])
        if i >= 2:
            finish(turns[i - 2])
    middle(turns[-1])
    finish(turns[-2])
    finish(turns[-1])

    for k in range(1, experts):
        arrivals[k, Z_OUT].wait_recv()

    def combine(n, carry):
        at_n = pl.ds(pl.multiple_of(n * cols, cols), cols)
        z = zrx[:, at_n]
        total = jnp.zeros((rows, cols), F32)
        for i in range(picks):
            total = total + gates[i] * jnp.dot(
                chosen[i], z, preferred_element_type=F32)
        out_ref[:, at_n] = total.astype(BF16)
        return carry

    lax.fori_loop(0, width // cols, combine, 0)
    for copy in copies.values():
        copy.wait_send()
    for copy in weights:
        copy.wait_send()


def per_device(tokens, norm_gain, expert_ids, gate_weights, w_gate, w_up, w_down):
    ep_devices = lax.axis_size("ep")
    rows, width = tokens.shape
    block = w_gate.shape[1]
    picks = expert_ids.shape[1]
    experts = ep_devices // GROUP
    capacity = max(2, min(rows, rows * picks * 4 // (3 * experts)))
    cap = -(-capacity // 16) * 16
    vmem = pl.BlockSpec(memory_space=pltpu.VMEM)
    hbm = pl.BlockSpec(memory_space=pl.ANY)
    chunk = GROUP * cap
    return pl.pallas_call(
        functools.partial(kernel, experts, cap, 256),
        out_shape=jax.ShapeDtypeStruct((rows, width), BF16),
        in_specs=[vmem] * 4 + [hbm] * 3,
        out_specs=vmem,
        scratch_shapes=[
            pltpu.VMEM((width, 2 * block), BF16),
            pltpu.VMEM((width, 2 * block), BF16),
            pltpu.VMEM((2 * block, width), BF16),
            pltpu.VMEM((experts * cap, width), BF16),
            pltpu.VMEM((experts, chunk, width), BF16),
            pltpu.VMEM((chunk, 2 * block), BF16),
            pltpu.VMEM((experts, chunk, width), BF16),
            pltpu.VMEM((experts, 2, cap, width), BF16),
            pltpu.VMEM((experts, cap, width), BF16),
            pltpu.VMEM((experts, cap, width), BF16),
            pltpu.VMEM((experts, cap, width), BF16),
            pltpu.VMEM((experts * cap, width), BF16),
            pltpu.SemaphoreType.DMA((experts * (COPIES + 2),)),
            pltpu.SemaphoreType.DMA((experts * COPIES,)),
            pltpu.SemaphoreType.DMA((3,)),
            pltpu.SemaphoreType.DMA((3,)),
            pltpu.SemaphoreType.DMA((3,)),
        ],
        compiler_params=pltpu.CompilerParams(
            collective_id=0, has_side_effects=True, vmem_limit_bytes=60 * 1024 * 1024),
    )(tokens, norm_gain.reshape(1, width), expert_ids.T, gate_weights.T, w_gate, w_up, w_down)


def solution(mesh):
    rows = P(("grp", "ep", "tp"), None)
    return jax.shard_map(
        per_device, mesh=mesh,
        in_specs=(rows, P(), rows, rows, P(None, ("ep", "tp")), P(None, ("ep", "tp")),
                  P(("ep", "tp"), None)),
        out_specs=rows, check_vma=False,
    )
```
